32 devices in a mesh: dp: 4 (over y, x), kv: 4 (over z), tp: 2 (over core).
Axes of the slice: x: 2, y: 2, z: 4, core: 2. Of those that a mesh axis runs over, the one named last changes fastest.
Arguments:
- tokens: bfloat16 [4, 16, 2048], P('dp', None, 'kv'), may hold values from -18 to 18, as said below
- norm_gain: float32 [2048], P('kv'), may hold values from 0.1 to 1.9
- w_query: bfloat16 [2048, 3072], P('kv', 'tp'), may hold values from -0.125 to 0.125
- w_key: bfloat16 [2048, 3072], P('kv', 'tp'), may hold values from -0.125 to 0.125
- w_value: bfloat16 [2048, 3072], P('kv', 'tp'), may hold values from -0.125 to 0.125
- w_gate: bfloat16 [2048, 3072], P('kv', 'tp'), may hold values from -0.125 to 0.125
- w_out: bfloat16 [3072, 2048], P('tp', 'kv'), may hold values from -0.109375 to 0.109375
- head_bias: float32 [24], P('tp'), may hold values from -14 to -2
- cache_keys: bfloat16 [4, 2048, 24, 128], P('dp', 'kv', 'tp'), may hold values from -18 to 18, as said below
- cache_values: bfloat16 [4, 2048, 24, 128], P('dp', 'kv', 'tp'), may hold values from -6 to 6
- prefix_len: int32 [4], P('dp'), may hold values from 1536 to 2028
- accepted: int32 [4], P('dp'), may hold values from 1 to 4
- parent: int32 [4, 16], P('dp'), may hold values from -1 to 14, as said below
Outputs:
- mixed: bfloat16 [4, 16, 2048], P('dp', None, 'kv')
- keys_next: bfloat16 [4, 2048, 24, 128], P('dp', 'kv', 'tp')
- values_next: bfloat16 [4, 2048, 24, 128], P('dp', 'kv', 'tp')
The draws below stay inside these ranges and needn't reach their ends.
Inputs may be any that keep to these rules, and one draw needn't show every extreme that they name: `tokens`: entries of order one. `cache_keys`: entries of order one. parent of proposal 0 is -1; for p of 1 or more, parent[p] lies in max(p - 3, 0) to p - 1.
All inputs are finite; a program needn't handle non-finite values.
Results may differ from the reference program's by a relative error of at most 0.012.
Values may be sent and summed in bfloat16 or wider, within the bound.
A program may use at most 64 MiB of HBM per device.

```python
import math
import jax
import jax.numpy as jnp
from jax import lax

D = 2048
HEADS = 24
HEAD = 128
BRANCH = 3072
PROPS = 16
LAST = 4
CTX = 2048
SEQS = 4
N_TP = 2


def draw_tokens(key, part):
    plain = jnp.clip(jax.random.normal(jax.random.fold_in(key, 11), (SEQS, PROPS, D), jnp.float32), -6.0, 6.0)
    blocks = (D + 63) // 64
    spread = jnp.exp(jax.random.uniform(jax.random.fold_in(key, 12), (1, 1, blocks), jnp.float32, math.log(0.3), math.log(3.0)))
    spread = jnp.repeat(spread, 64, axis=2)[:, :, :D]
    return (plain * spread).astype(jnp.bfloat16)


def draw_head_bias(key, part):
    lowest, highest = (-12.0, -2.0)
    return jax.random.uniform(jax.random.fold_in(key, 21), (HEADS,), jnp.float32, lowest, highest)


def draw_cache_keys(key, part):
    plain = jnp.clip(jax.random.normal(jax.random.fold_in(key, 31), (SEQS, CTX, HEADS, HEAD), jnp.float32), -6.0, 6.0)
    blocks = (CTX + 127) // 128
    spread = jnp.exp(jax.random.uniform(jax.random.fold_in(key, 32), (SEQS, blocks, HEADS, 1), jnp.float32, math.log(0.4), math.log(3.0)))
    spread = jnp.repeat(spread, 128, axis=1)[:, :CTX]
    return (plain * spread).astype(jnp.bfloat16)


def draw_parent(key, part):
    places = jnp.arange(PROPS, dtype=jnp.int32)
    back = jax.random.randint(jax.random.fold_in(key, 41), (SEQS, PROPS), 0, 3).astype(jnp.int32)
    chosen = jnp.maximum(places[None, :] - 1 - back, 0)
    return jnp.where(places[None, :] == 0, -1, chosen).astype(jnp.int32)


def set_ends(result, stream_key, smallest, high):
    shape = result.shape
    spot = [jax.random.randint(jax.random.fold_in(stream_key, axis), (), 0, shape[axis]) for axis in range(len(shape))]
    result = result.at[tuple(spot)].set(smallest)
    longest = shape.index(max(shape))
    spot[longest] = (spot[longest] + 1) % shape[longest]
    return result.at[tuple(spot)].set(high)


def levels(own_key, dims, cuts, least, top_value):
    factor_of, own = 1.0, jax.random.fold_in(own_key, 6)
    for position, parts in cuts:
        heights = jnp.exp(jax.random.uniform(jax.random.fold_in(own, position), (parts,), jnp.float32, least / len(cuts), top_value / len(cuts)))
        factor_of = factor_of * jnp.repeat(heights, dims[position] // parts).reshape([-1 if axis == position else 1 for axis in range(len(dims))])
    return factor_of


def gaussian(stream_key, shape, deviation, limit, shards=(), held_as=jnp.bfloat16):
    factor_of = levels(stream_key, shape, shards, -0.22, 0.18) if shards else 1.0
    values = jax.random.normal(stream_key, shape, jnp.float32) * deviation * factor_of
    return jnp.minimum(jnp.maximum(values, -limit), limit).astype(held_as)


def setup_inputs(seed: int = 0) -> dict:
    arg_keys = jax.random.split(jax.random.key(seed), 14)
    return {
        "tokens": draw_tokens(jax.random.fold_in(arg_keys[13], 71), 0),
        "norm_gain": jnp.clip(1.0 + 0.18 * jax.random.normal(arg_keys[1], (D,), jnp.float32), 0.1, 1.9),
        "w_query": gaussian(arg_keys[2], (D, BRANCH), D ** -0.5, 0.125, ((0, 4), (1, 2))),
        "w_key": gaussian(arg_keys[3], (D, BRANCH), D ** -0.5, 0.125, ((0, 4), (1, 2))),
        "w_value": gaussian(arg_keys[4], (D, BRANCH), D ** -0.5, 0.125, ((0, 4), (1, 2))),
        "w_gate": gaussian(arg_keys[5], (D, BRANCH), D ** -0.5, 0.125, ((0, 4), (1, 2))),
        "w_out": gaussian(arg_keys[6], (BRANCH, D), BRANCH ** -0.5, 0.109375, ((0, 2), (1, 4))),
        "head_bias": draw_head_bias(jax.random.fold_in(arg_keys[13], 71), 0),
        "cache_keys": draw_cache_keys(jax.random.fold_in(arg_keys[13], 71), 0),
        "cache_values": gaussian(arg_keys[9], (SEQS, CTX, HEADS, HEAD), 1.0, 6.0, ((0, 4), (1, 4), (2, 2))),
        "prefix_len": set_ends(jax.random.randint(arg_keys[10], (SEQS,), CTX - CTX // 4, CTX - PROPS - LAST + 1), jax.random.fold_in(arg_keys[10], 1), CTX - CTX // 4, CTX - PROPS - LAST).astype(jnp.int32),
        "accepted": set_ends(jax.random.randint(arg_keys[11], (SEQS,), 1, LAST + 1), jax.random.fold_in(arg_keys[11], 1), 1, LAST).astype(jnp.int32),
        "parent": draw_parent(jax.random.fold_in(arg_keys[13], 71), 0),
    }


EPS = 1e-06

def ancestry(parent):
    count = parent.shape[0]
    places = jnp.arange(count, dtype=jnp.int32)
    reach = (parent[:, None] == places[None, :]).astype(jnp.float32)
    for repeat in range(count.bit_length()):
        reach = jnp.minimum(reach + jnp.dot(reach, reach, precision=lax.Precision.HIGHEST), 1.0)
    return reach > 0.5

def one_sequence(packed, head_bias):
    query, key_new, value_new, cache_k, cache_v, valid, parent = packed
    factor = HEAD ** (-0.5)
    bias_col = head_bias[:, None, None]
    scores = jnp.einsum('phd,chd->hpc', query.astype(jnp.float32), cache_k.astype(jnp.float32)) * factor + bias_col
    live = (jnp.arange(cache_k.shape[0], dtype=jnp.int32) < valid)[None, None, :]
    keep_log = jnp.where(live, jax.nn.log_sigmoid(-scores), 0.0)
    family = ancestry(parent)[None]
    tree_scores = jnp.einsum('phd,jhd->hpj', query.astype(jnp.float32), key_new.astype(jnp.float32)) * factor + bias_col
    tree_keep = jnp.where(family, jax.nn.log_sigmoid(-tree_scores), 0.0)
    tail = lax.optimization_barrier(jnp.sum(tree_keep, axis=2, keepdims=True))
    later_cache = lax.cumsum(keep_log, axis=2, reverse=True) - keep_log + tail
    later_tree = lax.cumsum(tree_keep, axis=2, reverse=True) - tree_keep
    cache_weight = jnp.where(live, jnp.exp(jax.nn.log_sigmoid(scores) + later_cache), 0.0).astype(jnp.bfloat16)
    tree_weight = jnp.where(family, jnp.exp(jax.nn.log_sigmoid(tree_scores) + later_tree), 0.0).astype(jnp.bfloat16)
    attended = jnp.einsum('hpc,chd->phd', cache_weight.astype(jnp.float32), cache_v.astype(jnp.float32))
    attended = attended + jnp.einsum('hpj,jhd->phd', tree_weight.astype(jnp.float32), value_new.astype(jnp.float32))
    start = (valid.astype(jnp.int32), jnp.int32(0), jnp.int32(0))
    keys_next = lax.dynamic_update_slice(cache_k, key_new, start)
    values_next = lax.dynamic_update_slice(cache_v, value_new, start)
    return (attended, keys_next, values_next)

def reference(tokens, norm_gain, w_query, w_key, w_value, w_gate, w_out, head_bias, cache_keys, cache_values, prefix_len, accepted, parent):
    seqs, props, columns = tokens.shape
    flat = tokens.astype(jnp.float32).reshape(seqs * props, columns)
    squares = lax.optimization_barrier(jnp.sum(flat * flat, axis=1, keepdims=True))
    scaled = (flat * norm_gain).astype(jnp.bfloat16)
    rscale = lax.rsqrt(squares / columns + EPS)

    def project(weight):
        return (jnp.dot(scaled, weight, preferred_element_type=jnp.float32) * rscale).astype(jnp.bfloat16)
    query = project(w_query).reshape(seqs, props, HEADS, HEAD)
    key_new = project(w_key).reshape(seqs, props, HEADS, HEAD)
    value_new = project(w_value).reshape(seqs, props, HEADS, HEAD)
    gate = project(w_gate).astype(jnp.float32)
    valid = (prefix_len + accepted).astype(jnp.int32)
    attended, keys_next, values_next = lax.map(lambda packed: one_sequence(packed, head_bias), (query, key_new, value_new, cache_keys, cache_values, valid, parent))
    mixin = (attended.reshape(seqs * props, HEADS * HEAD) * jax.nn.silu(gate)).astype(jnp.bfloat16)
    group = HEADS * HEAD // N_TP
    total = jnp.zeros((seqs * props, columns), jnp.float32)
    for index in range(N_TP):
        part_out = jnp.dot(mixin[:, index * group:(index + 1) * group], w_out[index * group:(index + 1) * group], preferred_element_type=jnp.float32).astype(jnp.bfloat16)
        total = total + lax.optimization_barrier(part_out).astype(jnp.float32)
    mixed = total.astype(jnp.bfloat16).reshape(seqs, props, columns)
    return (mixed, keys_next, values_next)
```

```python
import functools

import jax
import jax.numpy as jnp
from jax import lax
from jax.experimental import pallas as pl
from jax.experimental.pallas import tpu as pltpu
from jax.sharding import PartitionSpec as P

D = 2048
HEAD = 128
LANES = 128
MESH = pl.DeviceIdType.MESH


EPS = 1e-06


def ancestry(parent):
    count = parent.shape[-1]
    places = jnp.arange(count, dtype=jnp.int32)
    reach = (parent[:, :, None] == places[None, None, :]).astype(jnp.float32)
    for repeat in range(count.bit_length()):
        reach = jnp.minimum(
            reach + jnp.einsum("spj,sjk->spk", reach, reach, precision=lax.Precision.HIGHEST), 1.0
        )
    return reach > 0.5


def after_table(count):
    places = jnp.arange(count, dtype=jnp.int32)
    return (places[:, None] > places[None, :]).astype(jnp.float32)


def sum_after(values):
    table = after_table(values.shape[-1])
    return jnp.einsum("shpk,kc->shpc", values, table, precision=lax.Precision.HIGHEST)


def local(
    tokens,
    norm_gain,
    w_query,
    w_key,
    w_value,
    w_gate,
    w_out,
    head_bias,
    cache_keys,
    cache_values,
    prefix_len,
    accepted,
    parent,
):
    seqs, props, columns = tokens.shape
    width = w_query.shape[1]
    heads = width // HEAD
    flat = tokens.astype(jnp.float32).reshape(seqs * props, columns)
    square_part = jnp.sum(flat * flat, axis=1)
    scaled = (flat * norm_gain).astype(jnp.bfloat16)
    partial_value = jnp.concatenate(
        [
            jnp.dot(scaled, weight, preferred_element_type=jnp.float32)
            for weight in (w_query, w_key, w_value, w_gate)
        ],
        axis=1,
    )
    squares = lax.psum(square_part, "kv")
    share = lax.psum_scatter(partial_value, "kv", scatter_dimension=1, tiled=True)
    rscale = lax.rsqrt(squares / D + EPS)
    projected = lax.all_gather(
        (share * rscale[:, None]).astype(jnp.bfloat16), "kv", axis=1, tiled=True
    )
    shaped = projected.reshape(seqs, props, 4, heads, HEAD)
    query = shaped[:, :, 0]
    key_new = shaped[:, :, 1]
    value_new = shaped[:, :, 2]
    gate = projected[:, 3 * width :].astype(jnp.float32)
    factor = HEAD ** (-0.5)
    bias_col = head_bias[None, :, None, None]
    ctx_dev = cache_keys.shape[1]
    places = lax.axis_index("kv") * ctx_dev + jnp.arange(ctx_dev, dtype=jnp.int32)
    valid = prefix_len + accepted
    live = (places[None, :] < valid[:, None])[:, None, None, :]
    scores = (
        jnp.einsum("sphd,schd->shpc", query, cache_keys, preferred_element_type=jnp.float32)
        * factor
        + bias_col
    )
    keep_log = jnp.where(live, jax.nn.log_sigmoid(-scores), 0.0)
    shard_rest = jnp.sum(keep_log, axis=3)
    family = ancestry(parent)[:, None]
    tree_scores = (
        jnp.einsum("sphd,sjhd->shpj", query, key_new, preferred_element_type=jnp.float32) * factor
        + bias_col
    )
    tree_keep = jnp.where(family, jax.nn.log_sigmoid(-tree_scores), 0.0)
    tail = jnp.sum(tree_keep, axis=3)
    every = lax.all_gather(shard_rest[None], "kv", axis=0, tiled=True)
    after = jnp.arange(every.shape[0], dtype=jnp.int32) > lax.axis_index("kv")
    beyond = jnp.sum(jnp.where(after[:, None, None, None], every, 0.0), axis=0)
    later_cache = sum_after(keep_log) + (beyond + tail)[..., None]
    cache_weight = jnp.where(live, jnp.exp(jax.nn.log_sigmoid(scores) + later_cache), 0.0).astype(
        jnp.bfloat16
    )
    later_tree = sum_after(tree_keep)
    tree_weight = jnp.where(
        family, jnp.exp(jax.nn.log_sigmoid(tree_scores) + later_tree), 0.0
    ).astype(jnp.bfloat16)
    local_sum = jnp.einsum(
        "shpc,schd->sphd", cache_weight, cache_values, preferred_element_type=jnp.float32
    )
    attended = lax.psum(local_sum, "kv")
    attended = attended + jnp.einsum(
        "shpj,sjhd->sphd", tree_weight, value_new, preferred_element_type=jnp.float32
    )
    mixin = (attended.reshape(seqs * props, width) * jax.nn.silu(gate)).astype(jnp.bfloat16)
    part_out = jnp.dot(mixin, w_out, preferred_element_type=jnp.float32).astype(jnp.bfloat16)
    part_out = lax.optimization_barrier(part_out).astype(jnp.float32)
    mixed = lax.psum(part_out.astype(jnp.bfloat16), "tp").reshape(seqs, props, w_out.shape[1])
    relative = places[None, :] - valid[:, None]
    picker = (relative[:, :, None] == jnp.arange(props, dtype=jnp.int32)[None, None, :]).astype(
        jnp.bfloat16
    )
    inside = ((relative >= 0) & (relative < props))[:, :, None, None]
    placed_keys = jnp.einsum(
        "scp,sphd->schd", picker, key_new, preferred_element_type=jnp.float32
    ).astype(jnp.bfloat16)
    placed_values = jnp.einsum(
        "scp,sphd->schd", picker, value_new, preferred_element_type=jnp.float32
    ).astype(jnp.bfloat16)
    keys_next = jnp.where(inside, placed_keys, cache_keys)
    values_next = jnp.where(inside, placed_values, cache_values)
    return (mixed, keys_next, values_next)


def softplus_tail(scores):
    return jnp.log1p(jnp.exp(-jnp.abs(scores)))


def three_parts(values):
    high = values.astype(jnp.bfloat16).astype(jnp.float32)
    rest = values - high
    middle = rest.astype(jnp.bfloat16).astype(jnp.float32)
    return high, middle, rest - middle


def lanes_of(columns, props):
    lane = lax.broadcasted_iota(jnp.int32, (props, LANES), 1)
    block = jnp.zeros((props, LANES), jnp.float32)
    for place, column in enumerate(columns):
        block = block + jnp.where(lane == place, column, 0.0)
    return block.astype(jnp.bfloat16)


def exchange_kernel(
    n_kv,
    first_writer,
    tokens_ref,
    gain_ref,
    wq_hbm,
    wk_hbm,
    wv_hbm,
    wg_hbm,
    wo_hbm,
    bias_ref,
    keys_hbm,
    values_hbm,
    prefix_ref,
    accepted_ref,
    parent_ref,
    parts_ref,
    fresh_ref,
    w_in,
    w_out,
    keys,
    values,
    partial,
    table,
    q_send,
    q_recv,
    q_own,
    q_all,
    p_send,
    p_recv,
    s_send,
    s_recv,
    m_send,
    m_recv,
    f_send,
    f_recv,
    o_recv,
    o_send,
    local_sem,
    send_sem,
    recv_sem,
):
    me = lax.axis_index("kv")
    core = lax.axis_index("tp")
    props, columns = tokens_ref.shape
    heads, ctx, head = keys.shape
    own = heads // n_kv
    group = own * head
    peers = [lax.rem(me + step, n_kv) for step in range(n_kv)]
    sources = [lax.rem(me + n_kv - step, n_kv) for step in range(n_kv)]

    barrier = pltpu.get_barrier_semaphore()
    for step in range(1, n_kv):
        pl.semaphore_signal(
            barrier, inc=1, device_id={"kv": peers[step]}, device_id_type=MESH
        )
    pl.semaphore_signal(barrier, inc=1, device_id={"tp": 1 - core}, device_id_type=MESH)

    loads = []
    for place, (src, dst) in enumerate(
        [
            (wq_hbm, w_in.at[0]),
            (wk_hbm, w_in.at[1]),
            (wv_hbm, w_in.at[2]),
            (wg_hbm, w_in.at[3]),
            (keys_hbm, keys),
            (values_hbm, values),
            (wo_hbm, w_out),
        ]
    ):
        copy = pltpu.make_async_copy(src, dst, local_sem.at[place])
        copy.start()
        loads.append(copy)

    started = []

    def send(kind, step, src, dst, device):
        copy = pltpu.make_async_remote_copy(
            src_ref=src,
            dst_ref=dst,
            send_sem=send_sem.at[kind, step],
            recv_sem=recv_sem.at[kind, step],
            device_id=device,
            device_id_type=MESH,
        )
        copy.start()
        return copy

    flat = tokens_ref[...].astype(jnp.float32)
    square_part = jnp.sum(flat * flat, axis=1, keepdims=True)
    scaled = (flat * gain_ref[...]).astype(jnp.bfloat16)
    square_lanes = lanes_of(three_parts(square_part), props)
    for owner in range(n_kv):
        q_send[owner, :, group:] = square_lanes

    def project(which):
        loads[which].wait()
        return jnp.dot(scaled, w_in[which], preferred_element_type=jnp.float32)

    part = project(0)
    for owner in range(n_kv):
        block = part[:, owner * group : (owner + 1) * group]
        partial[owner, :, :group] = block
        q_send[owner, :, :group] = block.astype(jnp.bfloat16)
    pl.semaphore_wait(barrier, n_kv)
    q_copies = [
        send(0, step, q_send.at[peers[step]], q_recv.at[step], {"kv": peers[step]})
        for step in range(n_kv - 1, 0, -1)
    ]
    started += q_copies

    for which in range(1, 4):
        part = project(which)
        for owner in range(n_kv):
            block = part[:, owner * group : (owner + 1) * group]
            partial[owner, :, which * group : (which + 1) * group] = block
            p_send[owner, :, (which - 1) * group : which * group] = block.astype(jnp.bfloat16)
    rows = lax.broadcasted_iota(jnp.int32, (ctx, ctx), 0)
    cols = lax.broadcasted_iota(jnp.int32, (ctx, ctx), 1)
    table[...] = jnp.where(rows > cols, 1.0, 0.0).astype(jnp.bfloat16)

    place_p = lax.broadcasted_iota(jnp.int32, (props, props), 0)
    place_j = lax.broadcasted_iota(jnp.int32, (props, props), 1)
    reach = jnp.where(parent_ref[...] == place_p, 1.0, 0.0)
    for repeat in range(props.bit_length()):
        reach = jnp.minimum(
            reach + jnp.dot(reach, reach, preferred_element_type=jnp.float32), 1.0
        )
    unit = jnp.where(place_p == place_j, 1.0, 0.0)
    reach = lax.dot_general(
        reach, unit, (((0,), (0,)), ((), ())), preferred_element_type=jnp.float32
    )
    family = jnp.concatenate([reach] * own, axis=0) > 0.5
    tree_table = jnp.where(place_p > place_j, 1.0, 0.0)

    total = partial[me, :, :group]
    squares = square_part
    for copy, step in zip(q_copies, range(n_kv - 1, 0, -1)):
        copy.wait_recv()
        total = total + q_recv[step, :, :group].astype(jnp.float32)
        lanes = q_recv[step, :, group:].astype(jnp.float32)
        squares = squares + (lanes[:, 0:1] + lanes[:, 1:2] + lanes[:, 2:3])
    rscale = lax.rsqrt(squares / (columns * n_kv) + EPS)
    q_mine = (total * rscale).astype(jnp.bfloat16)
    q_own[...] = q_mine
    a_copies = [
        send(1, step, q_own, q_all.at[step], {"kv": peers[step]})
        for step in range(n_kv - 1, 0, -1)
    ][::-1]
    started += a_copies
    p_copies = [
        send(2, step, p_send.at[peers[step]], p_recv.at[step], {"kv": peers[step]})
        for step in range(n_kv - 1, 0, -1)
    ]
    started += p_copies

    factor = head ** (-0.5)
    valid = prefix_ref[0] + accepted_ref[0]
    live = lax.broadcasted_iota(jnp.int32, (own * props, ctx), 1) + me * ctx < valid

    def attend(step):
        owner = sources[step]
        query = q_mine if step == 0 else q_all[step]
        scores = jnp.concatenate(
            [
                lax.dot_general(
                    query[:, each * head : (each + 1) * head],
                    keys[owner * own + each],
                    (((1,), (1,)), ((), ())),
                    preferred_element_type=jnp.float32,
                )
                * factor
                + bias_ref[owner * own + each]
                for each in range(own)
            ],
            axis=0,
        )
        soft = softplus_tail(scores)
        keep = jnp.where(live, -(jnp.maximum(scores, 0.0) + soft), 0.0)
        rest = jnp.sum(keep, axis=1, keepdims=True)
        high = keep.astype(jnp.bfloat16)
        low = (keep - high.astype(jnp.float32)).astype(jnp.bfloat16)
        later = jnp.dot(high, table[...], preferred_element_type=jnp.float32) + jnp.dot(
            low, table[...], preferred_element_type=jnp.float32
        )
        weight = jnp.where(live, jnp.exp(jnp.minimum(scores, 0.0) - soft + later), 0.0).astype(
            jnp.bfloat16
        )
        if step == 0:
            loads[5].wait()
        sums = [
            jnp.dot(
                weight[each * props : (each + 1) * props],
                values[owner * own + each],
                preferred_element_type=jnp.float32,
            )
            for each in range(own)
        ]
        rests = [rest[each * props : (each + 1) * props] for each in range(own)]
        return sums, rests

    loads[4].wait()
    sums_by, rests_by = [None] * n_kv, [None] * n_kv
    sums_by[0], rests_by[0] = attend(0)
    s_copies = [None] * n_kv
    for step in range(1, n_kv):
        a_copies[step - 1].wait_recv()
        sums, rests = attend(step)
        for each in range(own):
            s_send[step, :, each * head : (each + 1) * head] = sums[each].astype(jnp.bfloat16)
        pieces = [three_parts(rest) for rest in rests]
        s_send[step, :, group:] = lanes_of(
            [piece[level] for level in range(3) for piece in pieces], props
        )
        s_copies[step] = send(
            3, step, s_send.at[step], s_recv.at[step], {"kv": sources[step]}
        )
        started.append(s_copies[step])

    fresh = partial[me, :, group:]
    for copy, step in zip(p_copies, range(n_kv - 1, 0, -1)):
        copy.wait_recv()
        fresh = fresh + p_recv[step].astype(jnp.float32)
    fresh = (fresh * rscale).astype(jnp.bfloat16)
    key_new = fresh[:, :group]
    value_new = fresh[:, group : 2 * group]
    gate = fresh[:, 2 * group :].astype(jnp.float32)
    f_send[...] = fresh[:, : 2 * group]
    fresh_ref[...] = jnp.zeros_like(fresh_ref)
    fresh_ref[me] = fresh[:, : 2 * group]

    tree_scores = jnp.concatenate(
        [
            lax.dot_general(
                q_mine[:, each * head : (each + 1) * head],
                key_new[:, each * head : (each + 1) * head],
                (((1,), (1,)), ((), ())),
                preferred_element_type=jnp.float32,
            )
            * factor
            + bias_ref[me * own + each]
            for each in range(own)
        ],
        axis=0,
    )
    soft = softplus_tail(tree_scores)
    tree_keep = jnp.where(family, -(jnp.maximum(tree_scores, 0.0) + soft), 0.0)
    tail = jnp.sum(tree_keep, axis=1, keepdims=True)
    later = jnp.dot(
        tree_keep,
        tree_table,
        precision=lax.Precision.HIGHEST,
        preferred_element_type=jnp.float32,
    )
    tree_weight = jnp.where(
        family, jnp.exp(jnp.minimum(tree_scores, 0.0) - soft + later), 0.0
    ).astype(jnp.bfloat16)
    tree_sums = [
        jnp.dot(
            tree_weight[each * props : (each + 1) * props],
            value_new[:, each * head : (each + 1) * head],
            preferred_element_type=jnp.float32,
        )
        for each in range(own)
    ]
    silu = gate / (1.0 + jnp.exp(-gate))

    for step in range(1, n_kv):
        s_copies[step].wait_recv()
        lanes = s_recv[step, :, group:].astype(jnp.float32)
        rests_by[step] = [
            lanes[:, each : each + 1]
            + lanes[:, own + each : own + each + 1]
            + lanes[:, 2 * own + each : 2 * own + each + 1]
            for each in range(own)
        ]
        sums_by[step] = [
            s_recv[step, :, each * head : (each + 1) * head].astype(jnp.float32)
            for each in range(own)
        ]
    for each in range(own):
        attended = tree_sums[each]
        for step in range(n_kv):
            beyond = tail[each * props : (each + 1) * props]
            for other in range(n_kv):
                if other != step:
                    after = jnp.where(peers[other] > peers[step], 1.0, 0.0)
                    beyond = beyond + rests_by[other][each] * after
            attended = attended + jnp.exp(beyond) * sums_by[step][each]
        m_send[:, each * head : (each + 1) * head] = (
            attended * silu[:, each * head : (each + 1) * head]
        ).astype(jnp.bfloat16)
    m_copies = [
        send(4, step, m_send, m_recv.at[step], {"kv": peers[step]})
        for step in range(n_kv - 1, 0, -1)
    ][::-1]
    started += m_copies

    def hand(step):
        return pltpu.make_async_remote_copy(
            src_ref=f_send,
            dst_ref=f_recv.at[step],
            send_sem=send_sem.at[5, step],
            recv_sem=recv_sem.at[5, step],
            device_id={"kv": peers[step]},
            device_id_type=MESH,
        )

    for step in range(1, n_kv):

        @pl.when(peers[step] >= first_writer)
        def _(step=step):
            hand(step).start()

    loads[6].wait()

    def out_rows(step):
        start = pl.multiple_of(sources[step] * group, group)
        return w_out[pl.ds(start, group), :]

    mixed = jnp.dot(m_send[...], out_rows(0), preferred_element_type=jnp.float32)
    for step in range(1, n_kv):
        m_copies[step - 1].wait_recv()
        mixed = mixed + jnp.dot(
            m_recv[step], out_rows(step), preferred_element_type=jnp.float32
        )
    mixed = mixed.astype(jnp.bfloat16)
    o_send[...] = mixed
    o_copy = send(6, 0, o_send, o_recv, {"tp": 1 - core})
    parts_ref[0] = mixed

    @pl.when(me >= first_writer)
    def _():
        for step in range(1, n_kv):
            hand(step).wait_recv()
            fresh_ref[sources[step]] = f_recv[step]

    for copy in started:
        copy.wait_send()
    for step in range(1, n_kv):

        @pl.when(peers[step] >= first_writer)
        def _(step=step):
            hand(step).wait_send()

    o_copy.wait()
    parts_ref[1] = o_recv[...]


CHUNKS = 4


def cache_kernel(
    parts_ref,
    fresh_ref,
    prefix_ref,
    accepted_ref,
    keys_hbm,
    values_hbm,
    mixed_ref,
    keys_out,
    values_out,
    keys,
    values,
    in_sem,
    out_sem,
):
    heads, ctx, head = keys.shape
    n_kv, props, wide = fresh_ref.shape
    own = heads // n_kv
    step_heads = heads // CHUNKS
    pairs = []
    for chunk in range(CHUNKS):
        span = pl.ds(chunk * step_heads, step_heads)
        for side, (src, held, dst) in enumerate(
            [(keys_hbm, keys, keys_out), (values_hbm, values, values_out)]
        ):
            copy = pltpu.make_async_copy(
                src.at[span], held.at[span], in_sem.at[chunk, side]
            )
            copy.start()
            back = pltpu.make_async_copy(
                held.at[span], dst.at[span], out_sem.at[chunk, side]
            )
            pairs.append((chunk, side, held, copy, back))
    mixed_ref[...] = (
        parts_ref[0].astype(jnp.float32) + parts_ref[1].astype(jnp.float32)
    ).astype(jnp.bfloat16)
    start = prefix_ref[0] + accepted_ref[0] - lax.axis_index("kv") * ctx
    window = 2 * props
    base = pl.multiple_of(jnp.clip(start // props, 0, ctx // props - 2) * props, props)
    touched = (start + props > 0) & (start < ctx)
    row = lax.broadcasted_iota(jnp.int32, (window, props), 0) + base - start
    column = lax.broadcasted_iota(jnp.int32, (window, props), 1)
    picker = jnp.where(row == column, 1.0, 0.0).astype(jnp.bfloat16)
    offset = lax.broadcasted_iota(jnp.int32, (window, head), 0) + base - start
    inside = (offset >= 0) & (offset < props)
    for chunk, side, held, copy, back in pairs:
        copy.wait()

        @pl.when(touched)
        def _(chunk=chunk, side=side, held=held):
            for place in range(chunk * step_heads, (chunk + 1) * step_heads):
                at = side * own * head + (place % own) * head
                placed = jnp.dot(
                    picker,
                    fresh_ref[place // own, :, at : at + head],
                    preferred_element_type=jnp.float32,
                )
                now = held[place, pl.ds(base, window), :].astype(jnp.float32)
                held[place, pl.ds(base, window), :] = jnp.where(inside, placed, now).astype(
                    jnp.bfloat16
                )

        back.start()
    for chunk, side, held, copy, back in pairs:
        back.wait()


def fast(
    n_kv,
    tokens,
    norm_gain,
    w_query,
    w_key,
    w_value,
    w_gate,
    w_out,
    head_bias,
    cache_keys,
    cache_values,
    prefix_len,
    accepted,
    parent,
):
    _, props, columns = tokens.shape
    width = w_query.shape[1]
    heads = width // HEAD
    ctx = cache_keys.shape[1]
    out_columns = w_out.shape[1]
    group = width // n_kv
    whole = ctx * n_kv
    first_writer = (whole - whole // 4) // ctx
    keys = jnp.transpose(cache_keys[0], (1, 0, 2))
    values = jnp.transpose(cache_values[0], (1, 0, 2))
    vmem = pl.BlockSpec(memory_space=pltpu.VMEM)
    smem = pl.BlockSpec(memory_space=pltpu.SMEM)
    hbm = pl.BlockSpec(memory_space=pl.ANY)
    low = jnp.bfloat16
    cache_shape = (heads, ctx, HEAD)
    parts, fresh = pl.pallas_call(
        functools.partial(exchange_kernel, n_kv, first_writer),
        out_shape=(
            jax.ShapeDtypeStruct((2, props, out_columns), low),
            jax.ShapeDtypeStruct((n_kv, props, 2 * group), low),
        ),
        in_specs=[vmem, vmem, hbm, hbm, hbm, hbm, hbm, smem, hbm, hbm, smem, smem, vmem],
        out_specs=(vmem, vmem),
        scratch_shapes=[
            pltpu.VMEM((4, columns, width), low),
            pltpu.VMEM((width, out_columns), low),
            pltpu.VMEM(cache_shape, low),
            pltpu.VMEM(cache_shape, low),
            pltpu.VMEM((n_kv, props, 4 * group), jnp.float32),
            pltpu.VMEM((ctx, ctx), low),
            pltpu.VMEM((n_kv, props, group + LANES), low),
            pltpu.VMEM((n_kv, props, group + LANES), low),
            pltpu.VMEM((props, group), low),
            pltpu.VMEM((n_kv, props, group), low),
            pltpu.VMEM((n_kv, props, 3 * group), low),
            pltpu.VMEM((n_kv, props, 3 * group), low),
            pltpu.VMEM((n_kv, props, group + LANES), low),
            pltpu.VMEM((n_kv, props, group + LANES), low),
            pltpu.VMEM((props, group), low),
            pltpu.VMEM((n_kv, props, group), low),
            pltpu.VMEM((props, 2 * group), low),
            pltpu.VMEM((n_kv, props, 2 * group), low),
            pltpu.VMEM((props, out_columns), low),
            pltpu.VMEM((props, out_columns), low),
            pltpu.SemaphoreType.DMA((7,)),
            pltpu.SemaphoreType.DMA((7, n_kv)),
            pltpu.SemaphoreType.DMA((7, n_kv)),
        ],
        compiler_params=pltpu.CompilerParams(
            collective_id=0, has_side_effects=True, vmem_limit_bytes=40 * 1024 * 1024
        ),
        name="exchange",
    )(
        tokens[0],
        norm_gain[None],
        w_query,
        w_key,
        w_value,
        w_gate,
        w_out,
        head_bias,
        keys,
        values,
        prefix_len,
        accepted,
        parent,
    )
    mixed, keys_next, values_next = pl.pallas_call(
        cache_kernel,
        out_shape=(
            jax.ShapeDtypeStruct((props, out_columns), low),
            jax.ShapeDtypeStruct(cache_shape, low),
            jax.ShapeDtypeStruct(cache_shape, low),
        ),
        in_specs=[vmem, vmem, smem, smem, hbm, hbm],
        out_specs=(vmem, hbm, hbm),
        scratch_shapes=[
            pltpu.VMEM(cache_shape, low),
            pltpu.VMEM(cache_shape, low),
            pltpu.SemaphoreType.DMA((CHUNKS, 2)),
            pltpu.SemaphoreType.DMA((CHUNKS, 2)),
        ],
        compiler_params=pltpu.CompilerParams(vmem_limit_bytes=16 * 1024 * 1024),
        name="cache",
    )(parts, fresh, prefix_len, accepted, keys, values)
    return (
        mixed[None],
        jnp.transpose(keys_next, (1, 0, 2))[None],
        jnp.transpose(values_next, (1, 0, 2))[None],
    )


def solution(mesh):
    n_kv, n_tp = mesh.shape["kv"], mesh.shape["tp"]

    def body(*arrays):
        seqs, heads, ctx = arrays[0].shape[0], arrays[8].shape[2], arrays[8].shape[1]
        fits = heads % n_kv == 0 and heads % CHUNKS == 0 and seqs == 1 and n_tp == 2
        if fits and n_kv % 4 == 0 and ctx % 128 == 0:
            return fast(n_kv, *arrays)
        return local(*arrays)

    return jax.shard_map(
        body,
        mesh=mesh,
        in_specs=(
            P("dp", None, "kv"),
            P("kv"),
            P("kv", "tp"),
            P("kv", "tp"),
            P("kv", "tp"),
            P("kv", "tp"),
            P("tp", "kv"),
            P("tp"),
            P("dp", "kv", "tp", None),
            P("dp", "kv", "tp", None),
            P("dp"),
            P("dp"),
            P("dp", None),
        ),
        out_specs=(P("dp", None, "kv"), P("dp", "kv", "tp", None), P("dp", "kv", "tp", None)),
        check_vma=False,
    )
```

```python
import functools

import jax
import jax.numpy as jnp
from jax import lax
from jax.experimental import pallas as pl
from jax.experimental.pallas import tpu as pltpu
from jax.sharding import PartitionSpec as P

D = 2048
HEAD = 128
LANES = 128
SPLIT = 4
LIMIT = 50 * 1024 * 1024
MESH = pl.DeviceIdType.MESH


EPS = 1e-06


def ancestry(parent):
    count = parent.shape[-1]
    places = jnp.arange(count, dtype=jnp.int32)
    reach = (parent[:, :, None] == places[None, None, :]).astype(jnp.float32)
    for repeat in range(count.bit_length()):
        reach = jnp.minimum(
            reach + jnp.einsum("spj,sjk->spk", reach, reach, precision=lax.Precision.HIGHEST), 1.0
        )
    return reach > 0.5


def after_table(count):
    places = jnp.arange(count, dtype=jnp.int32)
    return (places[:, None] > places[None, :]).astype(jnp.float32)


def sum_after(values):
    table = after_table(values.shape[-1])
    return jnp.einsum("shpk,kc->shpc", values, table, precision=lax.Precision.HIGHEST)


def local(
    tokens,
    norm_gain,
    w_query,
    w_key,
    w_value,
    w_gate,
    w_out,
    head_bias,
    cache_keys,
    cache_values,
    prefix_len,
    accepted,
    parent,
):
    seqs, props, columns = tokens.shape
    width = w_query.shape[1]
    heads = width // HEAD
    flat = tokens.astype(jnp.float32).reshape(seqs * props, columns)
    square_part = jnp.sum(flat * flat, axis=1)
    scaled = (flat * norm_gain).astype(jnp.bfloat16)
    partial_value = jnp.concatenate(
        [
            jnp.dot(scaled, weight, preferred_element_type=jnp.float32)
            for weight in (w_query, w_key, w_value, w_gate)
        ],
        axis=1,
    )
    squares = lax.psum(square_part, "kv")
    share = lax.psum_scatter(partial_value, "kv", scatter_dimension=1, tiled=True)
    rscale = lax.rsqrt(squares / D + EPS)
    projected = lax.all_gather(
        (share * rscale[:, None]).astype(jnp.bfloat16), "kv", axis=1, tiled=True
    )
    shaped = projected.reshape(seqs, props, 4, heads, HEAD)
    query = shaped[:, :, 0]
    key_new = shaped[:, :, 1]
    value_new = shaped[:, :, 2]
    gate = projected[:, 3 * width :].astype(jnp.float32)
    factor = HEAD ** (-0.5)
    bias_col = head_bias[None, :, None, None]
    ctx_dev = cache_keys.shape[1]
    places = lax.axis_index("kv") * ctx_dev + jnp.arange(ctx_dev, dtype=jnp.int32)
    valid = prefix_len + accepted
    live = (places[None, :] < valid[:, None])[:, None, None, :]
    scores = (
        jnp.einsum("sphd,schd->shpc", query, cache_keys, preferred_element_type=jnp.float32)
        * factor
        + bias_col
    )
    keep_log = jnp.where(live, jax.nn.log_sigmoid(-scores), 0.0)
    shard_rest = jnp.sum(keep_log, axis=3)
    family = ancestry(parent)[:, None]
    tree_scores = (
        jnp.einsum("sphd,sjhd->shpj", query, key_new, preferred_element_type=jnp.float32) * factor
        + bias_col
    )
    tree_keep = jnp.where(family, jax.nn.log_sigmoid(-tree_scores), 0.0)
    tail = jnp.sum(tree_keep, axis=3)
    every = lax.all_gather(shard_rest[None], "kv", axis=0, tiled=True)
    after = jnp.arange(every.shape[0], dtype=jnp.int32) > lax.axis_index("kv")
    beyond = jnp.sum(jnp.where(after[:, None, None, None], every, 0.0), axis=0)
    later_cache = sum_after(keep_log) + (beyond + tail)[..., None]
    cache_weight = jnp.where(live, jnp.exp(jax.nn.log_sigmoid(scores) + later_cache), 0.0).astype(
        jnp.bfloat16
    )
    later_tree = sum_after(tree_keep)
    tree_weight = jnp.where(
        family, jnp.exp(jax.nn.log_sigmoid(tree_scores) + later_tree), 0.0
    ).astype(jnp.bfloat16)
    local_sum = jnp.einsum(
        "shpc,schd->sphd", cache_weight, cache_values, preferred_element_type=jnp.float32
    )
    attended = lax.psum(local_sum, "kv")
    attended = attended + jnp.einsum(
        "shpj,sjhd->sphd", tree_weight, value_new, preferred_element_type=jnp.float32
    )
    mixin = (attended.reshape(seqs * props, width) * jax.nn.silu(gate)).astype(jnp.bfloat16)
    part_out = jnp.dot(mixin, w_out, preferred_element_type=jnp.float32).astype(jnp.bfloat16)
    part_out = lax.optimization_barrier(part_out).astype(jnp.float32)
    mixed = lax.psum(part_out.astype(jnp.bfloat16), "tp").reshape(seqs, props, w_out.shape[1])
    relative = places[None, :] - valid[:, None]
    picker = (relative[:, :, None] == jnp.arange(props, dtype=jnp.int32)[None, None, :]).astype(
        jnp.bfloat16
    )
    inside = ((relative >= 0) & (relative < props))[:, :, None, None]
    placed_keys = jnp.einsum(
        "scp,sphd->schd", picker, key_new, preferred_element_type=jnp.float32
    ).astype(jnp.bfloat16)
    placed_values = jnp.einsum(
        "scp,sphd->schd", picker, value_new, preferred_element_type=jnp.float32
    ).astype(jnp.bfloat16)
    keys_next = jnp.where(inside, placed_keys, cache_keys)
    values_next = jnp.where(inside, placed_values, cache_values)
    return (mixed, keys_next, values_next)


def softplus_tail(scores):
    return jnp.log1p(jnp.exp(-jnp.abs(scores)))


def three_parts(values):
    high = values.astype(jnp.bfloat16).astype(jnp.float32)
    rest = values - high
    middle = rest.astype(jnp.bfloat16).astype(jnp.float32)
    return high, middle, rest - middle


def lanes_of(columns, props):
    lane = lax.broadcasted_iota(jnp.int32, (props, LANES), 1)
    block = jnp.zeros((props, LANES), jnp.float32)
    for place, column in enumerate(columns):
        block = block + jnp.where(lane == place, column, 0.0)
    return block.astype(jnp.bfloat16)


def exchange_kernel(
    n_kv,
    first_writer,
    tokens_hbm,
    gain_hbm,
    wq_hbm,
    wk_hbm,
    wv_hbm,
    wg_hbm,
    wo_hbm,
    bias_hbm,
    keys_hbm,
    values_hbm,
    prefix_hbm,
    accepted_hbm,
    parent_hbm,
    parts_ref,
    fresh_ref,
    keys,
    values,
    tokens_ref,
    gain_ref,
    parent_ref,
    bias_ref,
    prefix_ref,
    accepted_ref,
    w_in,
    w_out,
    partial,
    table,
    q_send,
    q_recv,
    q_own,
    q_all,
    p_send,
    p_recv,
    s_send,
    s_recv,
    m_send,
    m_recv,
    f_send,
    f_recv,
    o_recv,
    o_send,
    local_sem,
    send_sem,
    recv_sem,
):
    me = lax.axis_index("kv")
    core = lax.axis_index("tp")
    props, columns = tokens_ref.shape
    heads, ctx, head = keys.shape
    own = heads // n_kv
    group = own * head
    peers = [lax.rem(me + step, n_kv) for step in range(n_kv)]
    sources = [lax.rem(me + n_kv - step, n_kv) for step in range(n_kv)]

    barrier = pltpu.get_barrier_semaphore()
    for step in range(1, n_kv):
        pl.semaphore_signal(
            barrier, inc=1, device_id={"kv": peers[step]}, device_id_type=MESH
        )
    pl.semaphore_signal(barrier, inc=1, device_id={"tp": 1 - core}, device_id_type=MESH)

    def load(place, src, dst):
        copy = pltpu.make_async_copy(src, dst, local_sem.at[place])
        copy.start()
        return copy

    small = [load(7, tokens_hbm, tokens_ref), load(8, gain_hbm, gain_ref)]
    rows = columns // SPLIT
    first = []
    for piece in range(SPLIT):
        span = pl.ds(piece * rows, rows)
        first.append(load(13 + piece, wq_hbm.at[span], w_in.at[0, span]))
    late = [
        load(9, bias_hbm, bias_ref),
        load(10, prefix_hbm, prefix_ref),
        load(11, accepted_hbm, accepted_ref),
        load(12, parent_hbm, parent_ref),
    ]
    loads = [None] + [
        load(place, src, dst)
        for place, src, dst in [
            (1, wk_hbm, w_in.at[1]),
            (2, wv_hbm, w_in.at[2]),
            (3, wg_hbm, w_in.at[3]),
            (4, keys_hbm, keys),
            (5, values_hbm, values),
            (6, wo_hbm, w_out),
        ]
    ]

    started = []

    def send(kind, step, src, dst, device):
        copy = pltpu.make_async_remote_copy(
            src_ref=src,
            dst_ref=dst,
            send_sem=send_sem.at[kind, step],
            recv_sem=recv_sem.at[kind, step],
            device_id=device,
            device_id_type=MESH,
        )
        copy.start()
        return copy

    for copy in small:
        copy.wait()
    flat = tokens_ref[...].astype(jnp.float32)
    square_part = jnp.sum(flat * flat, axis=1, keepdims=True)
    scaled = (flat * gain_ref[...]).astype(jnp.bfloat16)
    square_lanes = lanes_of(three_parts(square_part), props)
    for owner in range(n_kv):
        q_send[owner, :, group:] = square_lanes

    def project(which):
        for copy in first if which == 0 else [loads[which]]:
            copy.wait()
        return jnp.dot(scaled, w_in[which], preferred_element_type=jnp.float32)

    part = project(0)
    for owner in range(n_kv):
        block = part[:, owner * group : (owner + 1) * group]
        partial[owner, :, :group] = block
        q_send[owner, :, :group] = block.astype(jnp.bfloat16)
    pl.semaphore_wait(barrier, n_kv)
    q_copies = [
        send(0, step, q_send.at[peers[step]], q_recv.at[step], {"kv": peers[step]})
        for step in range(n_kv - 1, 0, -1)
    ]
    started += q_copies

    for which in range(1, 4):
        part = project(which)
        for owner in range(n_kv):
            block = part[:, owner * group : (owner + 1) * group]
            partial[owner, :, which * group : (which + 1) * group] = block
            p_send[owner, :, (which - 1) * group : which * group] = block.astype(jnp.bfloat16)
    rows = lax.broadcasted_iota(jnp.int32, (ctx, ctx), 0)
    cols = lax.broadcasted_iota(jnp.int32, (ctx, ctx), 1)
    table[...] = jnp.where(rows > cols, 1.0, 0.0).astype(jnp.bfloat16)

    for copy in late:
        copy.wait()
    place_p = lax.broadcasted_iota(jnp.int32, (props, props), 0)
    place_j = lax.broadcasted_iota(jnp.int32, (props, props), 1)
    reach = jnp.where(parent_ref[...] == place_p, 1.0, 0.0)
    for repeat in range(props.bit_length()):
        reach = jnp.minimum(
            reach + jnp.dot(reach, reach, preferred_element_type=jnp.float32), 1.0
        )
    unit = jnp.where(place_p == place_j, 1.0, 0.0)
    reach = lax.dot_general(
        reach, unit, (((0,), (0,)), ((), ())), preferred_element_type=jnp.float32
    )
    family = jnp.concatenate([reach] * own, axis=0) > 0.5
    tree_table = jnp.where(place_p > place_j, 1.0, 0.0)

    total = partial[me, :, :group]
    squares = square_part
    for copy, step in zip(q_copies, range(n_kv - 1, 0, -1)):
        copy.wait_recv()
        total = total + q_recv[step, :, :group].astype(jnp.float32)
        lanes = q_recv[step, :, group:].astype(jnp.float32)
        squares = squares + (lanes[:, 0:1] + lanes[:, 1:2] + lanes[:, 2:3])
    rscale = lax.rsqrt(squares / (columns * n_kv) + EPS)
    q_mine = (total * rscale).astype(jnp.bfloat16)
    q_own[...] = q_mine
    a_copies = [
        send(1, step, q_own, q_all.at[step], {"kv": peers[step]})
        for step in range(n_kv - 1, 0, -1)
    ][::-1]
    started += a_copies
    p_copies = [
        send(2, step, p_send.at[peers[step]], p_recv.at[step], {"kv": peers[step]})
        for step in range(n_kv - 1, 0, -1)
    ]
    started += p_copies

    factor = head ** (-0.5)
    valid = prefix_ref[0] + accepted_ref[0]
    live = lax.broadcasted_iota(jnp.int32, (own * props, ctx), 1) + me * ctx < valid

    def attend(step):
        owner = sources[step]
        query = q_mine if step == 0 else q_all[step]
        scores = jnp.concatenate(
            [
                lax.dot_general(
                    query[:, each * head : (each + 1) * head],
                    keys[owner * own + each],
                    (((1,), (1,)), ((), ())),
                    preferred_element_type=jnp.float32,
                )
                * factor
                + bias_ref[owner * own + each]
                for each in range(own)
            ],
            axis=0,
        )
        soft = softplus_tail(scores)
        keep = jnp.where(live, -(jnp.maximum(scores, 0.0) + soft), 0.0)
        rest = jnp.sum(keep, axis=1, keepdims=True)
        high = keep.astype(jnp.bfloat16)
        low = (keep - high.astype(jnp.float32)).astype(jnp.bfloat16)
        later = jnp.dot(high, table[...], preferred_element_type=jnp.float32) + jnp.dot(
            low, table[...], preferred_element_type=jnp.float32
        )
        weight = jnp.where(live, jnp.exp(jnp.minimum(scores, 0.0) - soft + later), 0.0).astype(
            jnp.bfloat16
        )
        if step == 0:
            loads[5].wait()
        sums = [
            jnp.dot(
                weight[each * props : (each + 1) * props],
                values[owner * own + each],
                preferred_element_type=jnp.float32,
            )
            for each in range(own)
        ]
        rests = [rest[each * props : (each + 1) * props] for each in range(own)]
        return sums, rests

    loads[4].wait()
    sums_by, rests_by = [None] * n_kv, [None] * n_kv
    sums_by[0], rests_by[0] = attend(0)
    s_copies = [None] * n_kv
    for step in range(1, n_kv):
        a_copies[step - 1].wait_recv()
        sums, rests = attend(step)
        for each in range(own):
            s_send[step, :, each * head : (each + 1) * head] = sums[each].astype(jnp.bfloat16)
        pieces = [three_parts(rest) for rest in rests]
        s_send[step, :, group:] = lanes_of(
            [piece[level] for level in range(3) for piece in pieces], props
        )
        s_copies[step] = send(
            3, step, s_send.at[step], s_recv.at[step], {"kv": sources[step]}
        )
        started.append(s_copies[step])

    fresh = partial[me, :, group:]
    for copy, step in zip(p_copies, range(n_kv - 1, 0, -1)):
        copy.wait_recv()
        fresh = fresh + p_recv[step].astype(jnp.float32)
    fresh = (fresh * rscale).astype(jnp.bfloat16)
    key_new = fresh[:, :group]
    value_new = fresh[:, group : 2 * group]
    gate = fresh[:, 2 * group :].astype(jnp.float32)
    f_send[...] = fresh[:, : 2 * group]
    fresh_ref[...] = jnp.zeros_like(fresh_ref)
    fresh_ref[me] = fresh[:, : 2 * group]

    tree_scores = jnp.concatenate(
        [
            lax.dot_general(
                q_mine[:, each * head : (each + 1) * head],
                key_new[:, each * head : (each + 1) * head],
                (((1,), (1,)), ((), ())),
                preferred_element_type=jnp.float32,
            )
            * factor
            + bias_ref[me * own + each]
            for each in range(own)
        ],
        axis=0,
    )
    soft = softplus_tail(tree_scores)
    tree_keep = jnp.where(family, -(jnp.maximum(tree_scores, 0.0) + soft), 0.0)
    tail = jnp.sum(tree_keep, axis=1, keepdims=True)
    later = jnp.dot(
        tree_keep,
        tree_table,
        precision=lax.Precision.HIGHEST,
        preferred_element_type=jnp.float32,
    )
    tree_weight = jnp.where(
        family, jnp.exp(jnp.minimum(tree_scores, 0.0) - soft + later), 0.0
    ).astype(jnp.bfloat16)
    tree_sums = [
        jnp.dot(
            tree_weight[each * props : (each + 1) * props],
            value_new[:, each * head : (each + 1) * head],
            preferred_element_type=jnp.float32,
        )
        for each in range(own)
    ]
    silu = gate / (1.0 + jnp.exp(-gate))

    for step in range(1, n_kv):
        s_copies[step].wait_recv()
        lanes = s_recv[step, :, group:].astype(jnp.float32)
        rests_by[step] = [
            lanes[:, each : each + 1]
            + lanes[:, own + each : own + each + 1]
            + lanes[:, 2 * own + each : 2 * own + each + 1]
            for each in range(own)
        ]
        sums_by[step] = [
            s_recv[step, :, each * head : (each + 1) * head].astype(jnp.float32)
            for each in range(own)
        ]
    for each in range(own):
        attended = tree_sums[each]
        for step in range(n_kv):
            beyond = tail[each * props : (each + 1) * props]
            for other in range(n_kv):
                if other != step:
                    after = jnp.where(peers[other] > peers[step], 1.0, 0.0)
                    beyond = beyond + rests_by[other][each] * after
            attended = attended + jnp.exp(beyond) * sums_by[step][each]
        m_send[:, each * head : (each + 1) * head] = (
            attended * silu[:, each * head : (each + 1) * head]
        ).astype(jnp.bfloat16)
    m_copies = [
        send(4, step, m_send, m_recv.at[step], {"kv": peers[step]})
        for step in range(n_kv - 1, 0, -1)
    ][::-1]
    started += m_copies

    def hand(step):
        return pltpu.make_async_remote_copy(
            src_ref=f_send,
            dst_ref=f_recv.at[step],
            send_sem=send_sem.at[5, step],
            recv_sem=recv_sem.at[5, step],
            device_id={"kv": peers[step]},
            device_id_type=MESH,
        )

    for step in range(1, n_kv):

        @pl.when(peers[step] >= first_writer)
        def _(step=step):
            hand(step).start()

    loads[6].wait()

    def out_rows(step):
        start = pl.multiple_of(sources[step] * group, group)
        return w_out[pl.ds(start, group), :]

    mixed = jnp.dot(m_send[...], out_rows(0), preferred_element_type=jnp.float32)
    for step in range(1, n_kv):
        m_copies[step - 1].wait_recv()
        mixed = mixed + jnp.dot(
            m_recv[step], out_rows(step), preferred_element_type=jnp.float32
        )
    mixed = mixed.astype(jnp.bfloat16)
    o_send[...] = mixed
    o_copy = send(6, 0, o_send, o_recv, {"tp": 1 - core})
    parts_ref[0] = mixed

    @pl.when(me >= first_writer)
    def _():
        for step in range(1, n_kv):
            hand(step).wait_recv()
            fresh_ref[sources[step]] = f_recv[step]

    for copy in started:
        copy.wait_send()
    for step in range(1, n_kv):

        @pl.when(peers[step] >= first_writer)
        def _(step=step):
            hand(step).wait_send()

    o_copy.wait()
    parts_ref[1] = o_recv[...]


BLOCK = 64


def cache_kernel(
    parts_ref,
    fresh_ref,
    keys,
    values,
    prefix_hbm,
    accepted_hbm,
    mixed_ref,
    keys_out,
    values_out,
    patch,
    prefix_ref,
    accepted_ref,
    scalar_sem,
    out_sem,
    patch_sem,
):
    heads, ctx, head = keys.shape
    n_kv, props, wide = fresh_ref.shape
    own = heads // n_kv
    window = 2 * BLOCK
    blocks = ctx // BLOCK
    scalars = [
        pltpu.make_async_copy(prefix_hbm, prefix_ref, scalar_sem.at[0]),
        pltpu.make_async_copy(accepted_hbm, accepted_ref, scalar_sem.at[1]),
    ]
    for copy in scalars:
        copy.start()
    mixed_ref[...] = (
        parts_ref[0].astype(jnp.float32) + parts_ref[1].astype(jnp.float32)
    ).astype(jnp.bfloat16)
    for copy in scalars:
        copy.wait()
    start = prefix_ref[0] + accepted_ref[0] - lax.axis_index("kv") * ctx
    first = jnp.clip(start // BLOCK, 0, blocks - 2)
    base = pl.multiple_of(first * BLOCK, BLOCK)
    sides = [(keys, keys_out), (values, values_out)]

    def bulk(block, side):
        held, dst = sides[side]
        span = pl.ds(block * BLOCK, BLOCK)
        return pltpu.make_async_copy(
            held.at[:, span], dst.at[:, span], out_sem.at[block, side]
        )

    plain = [(block < first) | (block > first + 1) for block in range(blocks)]
    for block in range(blocks):

        @pl.when(plain[block])
        def _(block=block):
            for side in range(2):
                bulk(block, side).start()

    row = lax.broadcasted_iota(jnp.int32, (window, props), 0) + base - start
    column = lax.broadcasted_iota(jnp.int32, (window, props), 1)
    picker = jnp.where(row == column, 1.0, 0.0).astype(jnp.bfloat16)
    offset = lax.broadcasted_iota(jnp.int32, (window, head), 0) + base - start
    inside = (offset >= 0) & (offset < props)
    patches = []
    for side, (held, dst) in enumerate(sides):
        for place in range(heads):
            at = (side * own + place % own) * head
            placed = jnp.dot(
                picker,
                fresh_ref[place // own, :, at : at + head],
                preferred_element_type=jnp.float32,
            )
            now = held[place, pl.ds(base, window), :].astype(jnp.float32)
            patch[side, place] = jnp.where(inside, placed, now).astype(jnp.bfloat16)
        copy = pltpu.make_async_copy(
            patch.at[side], dst.at[:, pl.ds(base, window)], patch_sem.at[side]
        )
        copy.start()
        patches.append(copy)
    for block in range(blocks):

        @pl.when(plain[block])
        def _(block=block):
            for side in range(2):
                bulk(block, side).wait()

    for copy in patches:
        copy.wait()


def fast(
    n_kv,
    tokens,
    norm_gain,
    w_query,
    w_key,
    w_value,
    w_gate,
    w_out,
    head_bias,
    cache_keys,
    cache_values,
    prefix_len,
    accepted,
    parent,
):
    _, props, columns = tokens.shape
    width = w_query.shape[1]
    heads = width // HEAD
    ctx = cache_keys.shape[1]
    out_columns = w_out.shape[1]
    group = width // n_kv
    whole = ctx * n_kv
    first_writer = (whole - whole // 4) // ctx
    keys = jnp.transpose(cache_keys[0], (1, 0, 2))
    values = jnp.transpose(cache_values[0], (1, 0, 2))
    vmem = pl.BlockSpec(memory_space=pltpu.VMEM)
    hbm = pl.BlockSpec(memory_space=pl.ANY)
    low = jnp.bfloat16
    cache_shape = (heads, ctx, HEAD)
    parts, fresh, keys_held, values_held = pl.pallas_call(
        functools.partial(exchange_kernel, n_kv, first_writer),
        out_shape=(
            jax.ShapeDtypeStruct((2, props, out_columns), low),
            jax.ShapeDtypeStruct((n_kv, props, 2 * group), low),
            jax.ShapeDtypeStruct(cache_shape, low),
            jax.ShapeDtypeStruct(cache_shape, low),
        ),
        in_specs=[hbm] * 13,
        out_specs=(vmem,) * 4,
        scratch_shapes=[
            pltpu.VMEM((props, columns), low),
            pltpu.VMEM((1, columns), jnp.float32),
            pltpu.VMEM((1, props), jnp.int32),
            pltpu.SMEM((heads,), jnp.float32),
            pltpu.SMEM((1,), jnp.int32),
            pltpu.SMEM((1,), jnp.int32),
            pltpu.VMEM((4, columns, width), low),
            pltpu.VMEM((width, out_columns), low),
            pltpu.VMEM((n_kv, props, 4 * group), jnp.float32),
            pltpu.VMEM((ctx, ctx), low),
            pltpu.VMEM((n_kv, props, group + LANES), low),
            pltpu.VMEM((n_kv, props, group + LANES), low),
            pltpu.VMEM((props, group), low),
            pltpu.VMEM((n_kv, props, group), low),
            pltpu.VMEM((n_kv, props, 3 * group), low),
            pltpu.VMEM((n_kv, props, 3 * group), low),
            pltpu.VMEM((n_kv, props, group + LANES), low),
            pltpu.VMEM((n_kv, props, group + LANES), low),
            pltpu.VMEM((props, group), low),
            pltpu.VMEM((n_kv, props, group), low),
            pltpu.VMEM((props, 2 * group), low),
            pltpu.VMEM((n_kv, props, 2 * group), low),
            pltpu.VMEM((props, out_columns), low),
            pltpu.VMEM((props, out_columns), low),
            pltpu.SemaphoreType.DMA((13 + SPLIT,)),
            pltpu.SemaphoreType.DMA((7, n_kv)),
            pltpu.SemaphoreType.DMA((7, n_kv)),
        ],
        compiler_params=pltpu.CompilerParams(
            collective_id=0, has_side_effects=True, vmem_limit_bytes=LIMIT
        ),
        name="exchange",
    )(
        tokens[0],
        norm_gain[None],
        w_query,
        w_key,
        w_value,
        w_gate,
        w_out,
        head_bias,
        keys,
        values,
        prefix_len,
        accepted,
        parent,
    )
    mixed, keys_next, values_next = pl.pallas_call(
        cache_kernel,
        out_shape=(
            jax.ShapeDtypeStruct((props, out_columns), low),
            jax.ShapeDtypeStruct(cache_shape, low),
            jax.ShapeDtypeStruct(cache_shape, low),
        ),
        in_specs=[vmem] * 4 + [hbm] * 2,
        out_specs=(vmem, hbm, hbm),
        scratch_shapes=[
            pltpu.VMEM((2, heads, 2 * BLOCK, HEAD), low),
            pltpu.SMEM((1,), jnp.int32),
            pltpu.SMEM((1,), jnp.int32),
            pltpu.SemaphoreType.DMA((2,)),
            pltpu.SemaphoreType.DMA((ctx // BLOCK, 2)),
            pltpu.SemaphoreType.DMA((2,)),
        ],
        compiler_params=pltpu.CompilerParams(vmem_limit_bytes=16 * 1024 * 1024),
        name="cache",
    )(parts, fresh, keys_held, values_held, prefix_len, accepted)
    return (
        mixed[None],
        jnp.transpose(keys_next, (1, 0, 2))[None],
        jnp.transpose(values_next, (1, 0, 2))[None],
    )


def solution(mesh):
    n_kv, n_tp = mesh.shape["kv"], mesh.shape["tp"]

    def body(*arrays):
        seqs, heads, ctx = arrays[0].shape[0], arrays[8].shape[2], arrays[8].shape[1]
        fits = heads % n_kv == 0 and seqs == 1 and n_tp == 2
        if fits and n_kv % 4 == 0 and ctx % 128 == 0:
            return fast(n_kv, *arrays)
        return local(*arrays)

    return jax.shard_map(
        body,
        mesh=mesh,
        in_specs=(
            P("dp", None, "kv"),
            P("kv"),
            P("kv", "tp"),
            P("kv", "tp"),
            P("kv", "tp"),
            P("kv", "tp"),
            P("tp", "kv"),
            P("tp"),
            P("dp", "kv", "tp", None),
            P("dp", "kv", "tp", None),
            P("dp"),
            P("dp"),
            P("dp", None),
        ),
        out_specs=(P("dp", None, "kv"), P("dp", "kv", "tp", None), P("dp", "kv", "tp", None)),
        check_vma=False,
    )
```
